32 devices in a mesh: fs: 8 (over z, x), tp: 4 (over y, core).
Axes of the slice: x: 2, y: 2, z: 4, core: 2. Of those that a mesh axis runs over, the one named last changes fastest.
Arguments:
- tokens: bfloat16 [2048, 1536], P('fs', 'tp'), may hold values from -6 to 6
- norm_in_gain: float32 [1536], replicated, may hold values from 0.1 to 1.9
- query_w: bfloat16 [1536, 768], P('fs', 'tp'), may hold values from -0.15625 to 0.15625
- key_w: bfloat16 [1536, 768], P('fs', 'tp'), may hold values from -0.15625 to 0.15625
- value_w: bfloat16 [1536, 768], P('fs', 'tp'), may hold values from -0.15625 to 0.15625
- gate_w: bfloat16 [1536, 768], P('fs', 'tp'), may hold values from -0.15625 to 0.15625
- out_w: bfloat16 [768, 1536], P('tp', 'fs'), may hold values from -0.21875 to 0.21875
- norm_mid_gain: float32 [1536], replicated, may hold values from 0.1 to 1.9
- up_gate_w: bfloat16 [1536, 4096], P('fs', 'tp'), may hold values from -0.15625 to 0.15625
- up_value_w: bfloat16 [1536, 4096], P('fs', 'tp'), may hold values from -0.15625 to 0.15625
- conv_taps: float32 [3, 4096], P(None, 'tp'), may hold values from -3.5 to 3.5
- conv_bias: float32 [4096], P('tp'), may hold values from -3 to 3
- down_w: bfloat16 [4096, 1536], P('tp', 'fs'), may hold values from -0.09375 to 0.09375
Outputs:
- layer_out: bfloat16 [2048, 1536], P('fs', 'tp')
The draws below stay inside these ranges and needn't reach their ends.
All inputs are finite; a program needn't handle non-finite values.
Results may differ from the reference program's by a relative error of at most 0.02.
Values may be sent and summed in bfloat16 or wider, within the bound.
A program may use at most 64 MiB of HBM per device.

```python
import jax
import jax.numpy as jnp
from jax import lax

D = 1536
FF = 4096
HEADS = 8
BLOCK = 32
CONV = 3
TOK = 256
HEAD_DIM = 96
TOKENS = 2048
N_FS = 8


def shard_levels(stream_key, dims, split, low, high):
    gain = 1.0
    for dim, shards_of in split:
        draws = jax.random.uniform(jax.random.fold_in(jax.random.fold_in(stream_key, 6), dim), (shards_of,), jnp.float32, low / len(split), high / len(split))
        gain = gain * jnp.repeat(jnp.exp(draws), dims[dim] // shards_of).reshape((-1,) + (1,) * (len(dims) - 1 - dim))
    return gain


def normal_values(own_key, extent, spread, bound, cuts=(), kind=jnp.bfloat16):
    entries = spread * jax.random.normal(own_key, extent, jnp.float32)
    if cuts:
        entries = entries * shard_levels(own_key, extent, cuts, -0.22, 0.18)
    return jnp.clip(entries, -bound, bound).astype(kind)


def setup_inputs(seed: int = 0) -> dict:
    keys = jax.random.split(jax.random.key(seed), 14)
    return {
        "tokens": normal_values(keys[0], (TOKENS, D), 1.0, 6.0, ((0, 8), (1, 4))),
        "norm_in_gain": jnp.clip(1.0 + 0.18 * jax.random.normal(keys[1], (D,), jnp.float32), 0.1, 1.9),
        "query_w": normal_values(keys[2], (D, D // 2), D ** -0.5, 0.15625, ((0, 8), (1, 4))),
        "key_w": normal_values(keys[3], (D, D // 2), D ** -0.5, 0.15625, ((0, 8), (1, 4))),
        "value_w": normal_values(keys[4], (D, D // 2), D ** -0.5, 0.15625, ((0, 8), (1, 4))),
        "gate_w": normal_values(keys[5], (D, D // 2), D ** -0.5, 0.15625, ((0, 8), (1, 4))),
        "out_w": normal_values(keys[6], (D // 2, D), (D // 2) ** -0.5, 0.21875, ((0, 4), (1, 8))),
        "norm_mid_gain": jnp.clip(1.0 + 0.18 * jax.random.normal(keys[7], (D,), jnp.float32), 0.1, 1.9),
        "up_gate_w": normal_values(keys[8], (D, FF), D ** -0.5, 0.15625, ((0, 8), (1, 4))),
        "up_value_w": normal_values(keys[9], (D, FF), D ** -0.5, 0.15625, ((0, 8), (1, 4))),
        "conv_taps": normal_values(keys[10], (CONV, FF), CONV ** -0.5, 3.5, ((1, 4),), jnp.float32),
        "conv_bias": normal_values(keys[11], (FF,), 0.5, 3.0, ((0, 4),), jnp.float32),
        "down_w": normal_values(keys[12], (FF, D), FF ** -0.5, 0.09375, ((0, 4), (1, 8))),
    }


epsilon = 1e-06
rotary_base = 10000.0

def rms_scale(row_block, gain_row):
    widened = row_block.astype(jnp.float32)
    scaled = widened * lax.rsqrt(lax.optimization_barrier(jnp.mean(widened * widened, axis=-1, keepdims=True)) + epsilon)
    return (scaled * gain_row).astype(jnp.bfloat16)

def rotate(values_in, positions):
    half_width = values_in.shape[-1] // 2
    inv_freq = jnp.power(rotary_base, -jnp.arange(half_width, dtype=jnp.float32) / half_width)
    angles = positions[:, None] * inv_freq[None, :]
    cosine = jnp.cos(angles)[:, None, :]
    sine = jnp.sin(angles)[:, None, :]
    widened = values_in.astype(jnp.float32)
    first_half = widened[..., :half_width]
    second_half = widened[..., half_width:]
    return jnp.concatenate([first_half * cosine - second_half * sine, first_half * sine + second_half * cosine], axis=-1)

def retain(query_h, key_h, value_h, log_gamma, block_size):
    length, head_count, head_width = query_h.shape
    blocks = length // block_size
    offsets = jnp.arange(block_size, dtype=jnp.float32)
    lag_grid = offsets[:, None] - offsets[None, :]
    intra_decay = jnp.where(lag_grid[None] >= 0, jnp.exp(log_gamma[:, None, None] * jnp.maximum(lag_grid, 0.0)[None]), 0.0)
    query_decay = jnp.exp(log_gamma[None, :] * (offsets + 1.0)[:, None])
    key_decay = jnp.exp(log_gamma[None, :] * (block_size - 1.0 - offsets)[:, None])
    block_decay = jnp.exp(log_gamma * block_size)
    query_b = query_h.astype(jnp.float32).reshape(blocks, block_size, head_count, head_width)
    key_b = key_h.astype(jnp.float32).reshape(blocks, block_size, head_count, head_width)
    value_b = value_h.astype(jnp.float32).reshape(blocks, block_size, head_count, head_width)
    scores = jnp.einsum('nchd,nshd->nhcs', query_b, key_b, precision=lax.Precision.HIGHEST) * intra_decay[None]
    within = jnp.einsum('nhcs,nshe->nche', scores, value_b, precision=lax.Precision.HIGHEST)

    def advance(memory, block_inputs):
        query_n, key_n, value_n = block_inputs
        across_n = jnp.einsum('chd,hde->che', query_n * query_decay[:, :, None], memory, precision=lax.Precision.HIGHEST)
        memory = memory * block_decay[:, None, None] + jnp.einsum('chd,che->hde', key_n * key_decay[:, :, None], value_n, precision=lax.Precision.HIGHEST)
        return (memory, across_n)
    initial = jnp.zeros((head_count, head_width, head_width), jnp.float32)
    final_memory, across = lax.scan(advance, initial, (query_b, key_b, value_b))
    return (within + across).reshape(length, head_count, head_width)

def mix_heads(queries, key_m, value_m, gate_m, log_gamma, head_width, block_size):
    length = queries.shape[0]
    head_count = queries.shape[1] // head_width
    positions = jnp.arange(length, dtype=jnp.float32)
    query_r = rotate(queries.reshape(length, head_count, head_width), positions).astype(jnp.bfloat16)
    key_r = (rotate(key_m.reshape(length, head_count, head_width), positions) * head_width ** (-0.5)).astype(jnp.bfloat16)
    retained = retain(query_r, key_r, value_m.reshape(length, head_count, head_width), log_gamma, block_size)
    normed = retained * lax.rsqrt(lax.optimization_barrier(jnp.mean(retained * retained, axis=-1, keepdims=True)) + epsilon)
    return (normed.reshape(length, -1) * jax.nn.silu(gate_m.astype(jnp.float32))).astype(jnp.bfloat16)

def convolve(gate_up, conv_taps, conv_bias):
    length = gate_up.shape[0]
    tap_count = conv_taps.shape[0]
    padded = jnp.pad(gate_up.astype(jnp.float32), ((tap_count - 1, 0), (0, 0)))
    summed = jnp.zeros(gate_up.shape, jnp.float32) + conv_bias[None, :]
    for tap_index in range(tap_count):
        summed = summed + padded[tap_index:tap_index + length] * conv_taps[tap_index][None, :]
    return summed

def reference(tokens, norm_in_gain, query_w, key_w, value_w, gate_w, out_w, norm_mid_gain, up_gate_w, up_value_w, conv_taps, conv_bias, down_w):
    normed_in = rms_scale(tokens, norm_in_gain)

    def project(normed, weight):
        return jnp.dot(normed, weight, preferred_element_type=jnp.float32).astype(jnp.bfloat16)

    def by_sequence(matrix):
        return matrix.reshape(N_FS, TOK, matrix.shape[-1])
    queries = project(normed_in, query_w)
    key_m = project(normed_in, key_w)
    value_m = project(normed_in, value_w)
    gate_m = project(normed_in, gate_w)
    log_gamma = jnp.log1p(-jnp.exp2(-5.0 - jnp.arange(HEADS, dtype=jnp.float32)))
    gated_heads = jax.vmap(lambda q_part, k_part, v_part, g_part: mix_heads(q_part, k_part, v_part, g_part, log_gamma, HEAD_DIM, BLOCK))(by_sequence(queries), by_sequence(key_m), by_sequence(value_m), by_sequence(gate_m)).reshape(N_FS * TOK, -1)
    mixer_out = jnp.dot(gated_heads, out_w, preferred_element_type=jnp.float32)
    middle = (tokens.astype(jnp.float32) + mixer_out).astype(jnp.bfloat16)
    normed_mid = rms_scale(middle, norm_mid_gain)
    gate_up = project(normed_mid, up_gate_w)
    value_up = project(normed_mid, up_value_w)
    convolved = jax.vmap(lambda g_part: convolve(g_part, conv_taps, conv_bias))(by_sequence(gate_up)).reshape(N_FS * TOK, -1)
    hidden = (jax.nn.silu(convolved) * value_up.astype(jnp.float32)).astype(jnp.bfloat16)
    return (middle.astype(jnp.float32) + jnp.dot(hidden, down_w, preferred_element_type=jnp.float32)).astype(jnp.bfloat16)
```

```python
import jax
import jax.numpy as jnp
import numpy as np
from jax import lax
from jax.experimental import pallas as pl
from jax.experimental.pallas import tpu as pltpu
from jax.sharding import PartitionSpec as P

BLOCK = 32
HEAD_DIM = 96


epsilon = 1e-06
rotary_base = 10000.0


def taken_in(shard, axis, dim, absorb, state):
    everything = jax.tree.map(lambda a: lax.all_gather(a, axis, axis=dim, tiled=True), shard)
    return absorb(state, everything, jnp.int32(0))


def gathered_then(shard, axis, dim, block):
    whole = lax.all_gather(shard, axis, axis=dim, tiled=True)
    return block(whole, jnp.int32(0))


def rms_scale(row_block, gain_row):
    widened = row_block.astype(jnp.float32)
    scaled = widened * lax.rsqrt(jnp.mean(widened * widened, axis=-1, keepdims=True) + epsilon)
    return (scaled * gain_row).astype(jnp.bfloat16)


def rotate(values_in, positions):
    half_width = values_in.shape[-1] // 2
    inv_freq = jnp.power(rotary_base, -jnp.arange(half_width, dtype=jnp.float32) / half_width)
    angles = positions[:, None] * inv_freq[None, :]
    cosine = jnp.cos(angles)[:, None, :]
    sine = jnp.sin(angles)[:, None, :]
    widened = values_in.astype(jnp.float32)
    first_half = widened[..., :half_width]
    second_half = widened[..., half_width:]
    return jnp.concatenate(
        [first_half * cosine - second_half * sine, first_half * sine + second_half * cosine],
        axis=-1,
    )


def retain(query_h, key_h, value_h, log_gamma, block_size):
    length, head_count, head_width = query_h.shape
    blocks = length // block_size
    offsets = jnp.arange(block_size, dtype=jnp.float32)
    lag_grid = offsets[:, None] - offsets[None, :]
    intra_decay = jnp.where(
        lag_grid[None] >= 0,
        jnp.exp(log_gamma[:, None, None] * jnp.maximum(lag_grid, 0.0)[None]),
        0.0,
    )
    query_decay = jnp.exp(log_gamma[None, :] * (offsets + 1.0)[:, None])
    key_decay = jnp.exp(log_gamma[None, :] * (block_size - 1.0 - offsets)[:, None])
    block_decay = jnp.exp(log_gamma * block_size)
    query_b = query_h.astype(jnp.float32).reshape(blocks, block_size, head_count, head_width)
    key_b = key_h.astype(jnp.float32).reshape(blocks, block_size, head_count, head_width)
    value_b = value_h.astype(jnp.float32).reshape(blocks, block_size, head_count, head_width)
    scores = (
        jnp.einsum("nchd,nshd->nhcs", query_b, key_b, precision=lax.Precision.HIGHEST)
        * intra_decay[None]
    )
    within = jnp.einsum("nhcs,nshe->nche", scores, value_b, precision=lax.Precision.HIGHEST)

    def advance(memory, block_inputs):
        query_n, key_n, value_n = block_inputs
        across_n = jnp.einsum(
            "chd,hde->che",
            query_n * query_decay[:, :, None],
            memory,
            precision=lax.Precision.HIGHEST,
        )
        memory = memory * block_decay[:, None, None] + jnp.einsum(
            "chd,che->hde", key_n * key_decay[:, :, None], value_n, precision=lax.Precision.HIGHEST
        )
        return (memory, across_n)

    initial = jnp.zeros((head_count, head_width, head_width), jnp.float32)
    final_memory, across = lax.scan(advance, initial, (query_b, key_b, value_b))
    return (within + across).reshape(length, head_count, head_width)


def mix_heads(queries, key_m, value_m, gate_m, log_gamma, head_width, block_size):
    length = queries.shape[0]
    head_count = queries.shape[1] // head_width
    positions = jnp.arange(length, dtype=jnp.float32)
    query_r = rotate(queries.reshape(length, head_count, head_width), positions).astype(
        jnp.bfloat16
    )
    key_r = (
        rotate(key_m.reshape(length, head_count, head_width), positions) * head_width ** (-0.5)
    ).astype(jnp.bfloat16)
    retained = retain(
        query_r, key_r, value_m.reshape(length, head_count, head_width), log_gamma, block_size
    )
    normed = retained * lax.rsqrt(jnp.mean(retained * retained, axis=-1, keepdims=True) + epsilon)
    return (normed.reshape(length, -1) * jax.nn.silu(gate_m.astype(jnp.float32))).astype(
        jnp.bfloat16
    )


def convolve(gate_up, conv_taps, conv_bias):
    length = gate_up.shape[0]
    tap_count = conv_taps.shape[0]
    padded = jnp.pad(gate_up.astype(jnp.float32), ((tap_count - 1, 0), (0, 0)))
    summed = jnp.zeros(gate_up.shape, jnp.float32) + conv_bias[None, :]
    for tap_index in range(tap_count):
        summed = summed + padded[tap_index : tap_index + length] * conv_taps[tap_index][None, :]
    return summed


def single(normed):

    def add_single(running, weight_piece, row_start):
        columns = lax.dynamic_slice_in_dim(normed, row_start, weight_piece.shape[0], 1)
        return running + jnp.dot(columns, weight_piece, preferred_element_type=jnp.float32)

    return add_single


def features(shard):
    return lax.all_gather(shard, "tp", axis=1, tiled=True)


def head_sum(terms):
    return lax.psum_scatter(
        terms.astype(jnp.bfloat16), "tp", scatter_dimension=1, tiled=True
    ).astype(jnp.float32)


def local(
    tokens,
    norm_in_gain,
    query_w,
    key_w,
    value_w,
    gate_w,
    out_w,
    norm_mid_gain,
    up_gate_w,
    up_value_w,
    conv_taps,
    conv_bias,
    down_w,
):
    normed_in = rms_scale(features(tokens), norm_in_gain)
    length = normed_in.shape[0]

    def empty(weight):
        return jnp.zeros((length, weight.shape[1]), jnp.float32)

    add_in = single(normed_in)

    def mixer_row(weight):
        return taken_in(weight, "fs", 0, add_in, empty(weight))

    queries = mixer_row(query_w)
    key_m = mixer_row(key_w)
    value_m = mixer_row(value_w)
    gate_m = mixer_row(gate_w)
    head_count = query_w.shape[1] // HEAD_DIM
    first_head = lax.axis_index("tp") * head_count
    head_ids = (first_head + jnp.arange(head_count, dtype=jnp.int32)).astype(jnp.float32)
    log_gamma = jnp.log1p(-jnp.exp2(-5.0 - head_ids))
    gated_heads = mix_heads(
        queries.astype(jnp.bfloat16),
        key_m.astype(jnp.bfloat16),
        value_m.astype(jnp.bfloat16),
        gate_m.astype(jnp.bfloat16),
        log_gamma,
        HEAD_DIM,
        BLOCK,
    )

    def mixer_project(weight_piece, row_start):
        return jnp.dot(gated_heads, weight_piece, preferred_element_type=jnp.float32)

    mixer_terms = gathered_then(out_w, "fs", 1, mixer_project)
    middle = (tokens.astype(jnp.float32) + head_sum(mixer_terms)).astype(jnp.bfloat16)
    normed_mid = rms_scale(features(middle), norm_mid_gain)
    add_mid = single(normed_mid)

    def channel_row(weight):
        return taken_in(weight, "fs", 0, add_mid, empty(weight))

    gate_up = channel_row(up_gate_w)
    value_up = channel_row(up_value_w)
    convolved = convolve(gate_up.astype(jnp.bfloat16), conv_taps, conv_bias)
    hidden = (jax.nn.silu(convolved) * value_up.astype(jnp.bfloat16).astype(jnp.float32)).astype(
        jnp.bfloat16
    )

    def channel_project(weight_piece, row_start):
        return jnp.dot(hidden, weight_piece, preferred_element_type=jnp.float32)

    channel_terms = gathered_then(down_w, "fs", 1, channel_project)
    return (middle.astype(jnp.float32) + head_sum(channel_terms)).astype(jnp.bfloat16)


LANES = 128
MESH = pl.DeviceIdType.MESH


def padded_lanes(piece):
    return jnp.pad(piece, ((0, 0), (0, LANES - piece.shape[1])))


def dot(left, right):
    return jnp.dot(left, right, preferred_element_type=jnp.float32)


def dot_t(left, right):
    return lax.dot_general(left, right, (((1,), (1,)), ((), ())), preferred_element_type=jnp.float32)


def layer_kernel(
    fs_count,
    heads,
    tokens_ref,
    gain_in_ref,
    gain_mid_ref,
    wa_ref,
    wg_ref,
    wv_ref,
    wd_ref,
    taps_ref,
    bias_ref,
    cos_ref,
    sin_ref,
    turn_ref,
    out_ref,
    ga,
    gg,
    gv,
    gd,
    tok_all,
    mid_all,
    part_mix,
    part_ch,
    land_mix,
    land_ch,
    normed,
    w_send,
    w_recv,
    w_own,
    ag_send,
    ag_recv,
    ag_own,
    rs_send,
    rs_recv,
    hidden_gate,
    hidden,
    middle,
):
    fs = lax.axis_index("fs")
    tp = lax.axis_index("tp")
    z, x = fs // 2, fs % 2
    y, c = tp // 2, tp % 2
    zl = z % 2
    z_count = fs_count // 2
    rows, width = tokens_ref.shape
    depth = wa_ref.shape[1]
    tp_count = 4
    z_mate = (z + 1 - 2 * zl) * 2 + x
    x_mate = z * 2 + 1 - x
    y_mate = (1 - y) * 2 + c
    c_mate = y * 2 + 1 - c
    to_z, to_x, to_y, to_c = (z_mate, tp), (x_mate, tp), (fs, y_mate), (fs, c_mate)
    z_peers = [lax.rem(z + step, z_count) for step in range(1, z_count)]

    barrier = pltpu.get_barrier_semaphore()
    greeted = [(zp * 2 + x, tp) for zp in z_peers] + [to_x, to_y, to_c]
    for peer in greeted:
        pl.semaphore_signal(barrier, inc=1, device_id=peer, device_id_type=MESH)
    pl.semaphore_wait(barrier, len(greeted))

    sends = []

    def remote(src, dst, send_sem, recv_sem, peer):
        copy = pltpu.make_async_remote_copy(
            src_ref=src,
            dst_ref=dst,
            send_sem=send_sem,
            recv_sem=recv_sem,
            device_id=peer,
            device_id_type=MESH,
        )
        copy.start()
        sends.append(copy)

    def arrived(ref, sem):
        pltpu.make_async_remote_copy(
            src_ref=ref,
            dst_ref=ref,
            send_sem=sem,
            recv_sem=sem,
            device_id=to_c,
            device_id_type=MESH,
        ).wait_recv()

    def slot(held, owner):
        return held.at[pl.ds(pl.multiple_of(owner * depth, depth), depth)]

    chunks = [(wa_ref, ga), (wg_ref, gg), (wv_ref, gv), (wd_ref, gd)]
    own_copies = []

    def weights_out(k):
        shard, held = chunks[k]
        for i, zp in enumerate(z_peers):
            remote(
                shard.at[zp % 2],
                slot(held, fs),
                w_send.at[k, i],
                w_recv.at[k, fs],
                (zp * 2 + x, tp),
            )
        remote(
            shard.at[zl], slot(held, fs), w_send.at[k, z_count - 1], w_recv.at[k, fs], to_x
        )
        own = pltpu.make_async_copy(shard.at[zl], slot(held, fs), w_own.at[k])
        own.start()
        own_copies.append(own)

    def weights_on(k):
        held = chunks[k][1]
        for i in range(z_count - 1):
            owner = lax.rem(z + z_count - 1 - i, z_count) * 2 + x
            arrived(slot(held, owner), w_recv.at[k, owner])
            remote(
                slot(held, owner),
                slot(held, owner),
                w_send.at[k, z_count + i],
                w_recv.at[k, owner],
                to_x,
            )

    def weights_in(k):
        held = chunks[k][1]
        own_copies[k].wait()
        for step in range(z_count):
            owner = lax.rem(z + z_count - step, z_count) * 2 + 1 - x
            arrived(slot(held, owner), w_recv.at[k, owner])

    mine = zl * 4 + tp
    from_z = (1 - zl) * 4 + tp
    from_y = zl * 4 + y_mate
    from_zy = (1 - zl) * 4 + y_mate
    gathered = (mine, from_z, from_y, from_zy)

    def gather_start(phase, src, held):
        def pass_on(which, ref, block, peer):
            remote(
                ref, held.at[block], ag_send.at[phase, which], ag_recv.at[phase, block], peer
            )

        pass_on(0, src, mine, to_z)
        pass_on(1, src, mine, to_y)
        pass_on(2, src, mine, to_c)
        own = pltpu.make_async_copy(src, held.at[mine], ag_own.at[phase])
        own.start()
        return pass_on, own

    def gather_end(phase, held, state):
        pass_on, own = state
        arrived(held.at[from_z], ag_recv.at[phase, from_z])
        pass_on(3, held.at[from_z], from_z, to_y)
        pass_on(4, held.at[from_z], from_z, to_c)
        arrived(held.at[from_y], ag_recv.at[phase, from_y])
        pass_on(5, held.at[from_y], from_y, to_c)
        arrived(held.at[from_zy], ag_recv.at[phase, from_zy])
        pass_on(6, held.at[from_zy], from_zy, to_c)
        own.wait()
        for half in range(2):
            for side in range(2):
                block = half * 4 + side * 2 + 1 - c
                arrived(held.at[block], ag_recv.at[phase, block])

    def add_into(parts, block, land, where):
        parts[block] = (
            parts[block].astype(jnp.float32) + land[where].astype(jnp.float32)
        ).astype(jnp.bfloat16)

    def scatter(phase, parts, land, between):
        def give(which, block, peer):
            remote(
                parts.at[block],
                land.at[which],
                rs_send.at[phase, which],
                rs_recv.at[phase, which],
                peer,
            )

        def take(which):
            arrived(land.at[which], rs_recv.at[phase, which])

        for side in (1 - y, y):
            for half in (1 - zl, zl):
                give(half * 2 + side, half * 4 + side * 2 + 1 - c, to_c)
        for half in (1 - zl, zl):
            which = half * 2 + 1 - y
            take(which)
            block = half * 4 + (1 - y) * 2 + c
            add_into(parts, block, land, which)
            give(4 + half, block, to_y)
        between()
        for half in (1 - zl, zl):
            which = half * 2 + y
            take(which)
            add_into(parts, half * 4 + tp, land, which)
        take(4 + 1 - zl)
        add_into(parts, from_z, land, 4 + 1 - zl)
        give(6, from_z, to_z)
        take(4 + zl)
        total = parts[mine].astype(jnp.float32) + land[4 + zl].astype(jnp.float32)
        take(6)
        return total + land[6].astype(jnp.float32)

    def normalise(held, gain_ref):
        @pl.loop(0, 2)
        def _(half):
            squares = jnp.zeros((rows, 1), jnp.float32)
            for t in range(tp_count):
                wide = held[half * 4 + t].astype(jnp.float32)
                squares = squares + jnp.sum(wide * wide, axis=-1, keepdims=True)
            scale = lax.rsqrt(squares / (tp_count * width) + epsilon)
            for t in range(tp_count):
                wide = held[half * 4 + t].astype(jnp.float32)
                normed[half * 4 + t] = (
                    wide * scale * gain_ref[:, t * width : (t + 1) * width]
                ).astype(jnp.bfloat16)

    def project(half, held, columns):
        total = dot(normed[half * 4], held[0:width, 0:columns])
        for t in range(1, tp_count):
            total = total + dot(
                normed[half * 4 + t], held[t * width : (t + 1) * width, 0:columns]
            )
        return total.astype(jnp.bfloat16)

    state = gather_start(0, tokens_ref, tok_all)
    weights_out(0)
    weights_out(1)
    gather_end(0, tok_all, state)
    normalise(tok_all, gain_in_ref)
    weights_on(0)
    weights_out(2)
    weights_in(0)

    head = tp * 2 + zl
    log_gamma = jnp.float32(0.0)
    for j in range(heads):
        log_gamma = jnp.where(head == j, jnp.float32(np.log1p(-(2.0 ** (-5.0 - j)))), log_gamma)

    @pl.loop(0, 2)
    def _(half):
        wide = project(half, ga, 4 * LANES)
        turn = turn_ref[...]

        def rotated(piece):
            return piece.astype(jnp.float32) * cos_ref[...] + dot(piece, turn) * sin_ref[...]

        query_r = rotated(wide[:, 0:LANES]).astype(jnp.bfloat16)
        key_r = (rotated(wide[:, LANES : 2 * LANES]) * HEAD_DIM ** (-0.5)).astype(jnp.bfloat16)
        value = wide[:, 2 * LANES : 3 * LANES]
        gate = wide[:, 3 * LANES : 4 * LANES].astype(jnp.float32)
        later = lax.broadcasted_iota(jnp.int32, (rows, rows), 0)
        earlier = lax.broadcasted_iota(jnp.int32, (rows, rows), 1)
        lag = later - earlier
        decay = jnp.where(
            lag >= 0, jnp.exp(log_gamma * jnp.maximum(lag, 0).astype(jnp.float32)), 0.0
        )
        scores = dot_t(query_r, key_r) * decay
        coarse = scores.astype(jnp.bfloat16)
        fine = (scores - coarse.astype(jnp.float32)).astype(jnp.bfloat16)
        retained = dot(coarse, value) + dot(fine, value)
        square = jnp.sum(retained * retained, axis=-1, keepdims=True) / HEAD_DIM
        gated = (
            retained * lax.rsqrt(square + epsilon) * (gate * (1.0 / (1.0 + jnp.exp(-gate))))
        ).astype(jnp.bfloat16)
        for t in range(tp_count):
            part_mix[half * 4 + t] = dot_t(
                gated, ga[t * width : (t + 1) * width, 4 * LANES : 5 * LANES]
            ).astype(jnp.bfloat16)

    mixed = scatter(0, part_mix, land_mix, lambda: weights_on(1))
    middle[...] = (tokens_ref[...].astype(jnp.float32) + mixed).astype(jnp.bfloat16)
    state = gather_start(1, middle, mid_all)
    weights_out(3)
    gather_end(1, mid_all, state)
    weights_on(2)
    normalise(mid_all, gain_mid_ref)
    weights_in(1)

    @pl.loop(0, 2)
    def _(half):
        up = project(half, gg, gg.shape[1]).astype(jnp.float32)
        at = lax.broadcasted_iota(jnp.int32, up.shape, 0)
        taps = taps_ref[zl]
        tap_count = taps.shape[0]
        summed = up * taps[tap_count - 1 : tap_count] + bias_ref[zl]
        for back in range(1, tap_count):
            moved = jnp.where(at >= back, pltpu.roll(up, back, 0), 0.0)
            summed = summed + moved * taps[tap_count - 1 - back : tap_count - back]
        hidden_gate[half] = summed * (1.0 / (1.0 + jnp.exp(-summed)))

    weights_on(3)
    weights_in(2)

    @pl.loop(0, 2)
    def _(half):
        value_up = project(half, gv, gv.shape[1]).astype(jnp.float32)
        hidden[half] = (hidden_gate[half] * value_up).astype(jnp.bfloat16)

    weights_in(3)

    @pl.loop(0, 2)
    def _(half):
        for t in range(tp_count):
            part_ch[half * 4 + t] = dot_t(
                hidden[half], gd[t * width : (t + 1) * width]
            ).astype(jnp.bfloat16)

    summed = scatter(1, part_ch, land_ch, lambda: None)
    result = (middle[...].astype(jnp.float32) + summed).astype(jnp.bfloat16)
    for copy in sends:
        copy.wait_send()
    out_ref[...] = result


def rotation_tables(length):
    half_width = HEAD_DIM // 2
    inv_freq = rotary_base ** (-np.arange(half_width) / half_width)
    angles = np.arange(length)[:, None] * inv_freq[None, :]
    angles = np.pad(np.concatenate([angles, angles], axis=1), ((0, 0), (0, LANES - HEAD_DIM)))
    turn = np.zeros((LANES, LANES), np.float32)
    for i in range(half_width):
        turn[i + half_width, i] = -1.0
        turn[i, i + half_width] = 1.0
    return np.cos(angles).astype(np.float32), np.sin(angles).astype(np.float32), turn


def fused(
    fs_count,
    heads,
    tokens,
    norm_in_gain,
    query_w,
    key_w,
    value_w,
    gate_w,
    out_w,
    norm_mid_gain,
    up_gate_w,
    up_value_w,
    conv_taps,
    conv_bias,
    down_w,
):
    rows, width = tokens.shape
    hidden_half = up_gate_w.shape[1] // 2

    def of_half(b):
        head = slice(b * HEAD_DIM, (b + 1) * HEAD_DIM)
        pieces = [padded_lanes(w[:, head]) for w in (query_w, key_w, value_w, gate_w)]
        return jnp.concatenate(pieces + [padded_lanes(out_w[head].T)], axis=1)

    wa = jnp.stack([of_half(0), of_half(1)])
    wg = jnp.stack([up_gate_w[:, :hidden_half], up_gate_w[:, hidden_half:]])
    wv = jnp.stack([up_value_w[:, :hidden_half], up_value_w[:, hidden_half:]])
    wd = jnp.stack([down_w[:hidden_half].T, down_w[hidden_half:].T])
    taps = jnp.stack([conv_taps[:, :hidden_half], conv_taps[:, hidden_half:]])
    bias = conv_bias.reshape(2, 1, hidden_half)
    cosine, sine, turn = rotation_tables(rows)
    features_all = wa.shape[1] * fs_count
    block = (rows, width)

    def held(shard):
        return pltpu.VMEM((features_all, shard.shape[2]), jnp.bfloat16)

    z_count = fs_count // 2
    return pl.pallas_call(
        lambda *refs: layer_kernel(fs_count, heads, *refs),
        out_shape=jax.ShapeDtypeStruct(block, jnp.bfloat16),
        in_specs=[pl.BlockSpec(memory_space=pltpu.VMEM)] * 12,
        out_specs=pl.BlockSpec(memory_space=pltpu.VMEM),
        scratch_shapes=[
            held(wa),
            held(wg),
            held(wv),
            held(wd),
            pltpu.VMEM((8,) + block, jnp.bfloat16),
            pltpu.VMEM((8,) + block, jnp.bfloat16),
            pltpu.VMEM((8,) + block, jnp.bfloat16),
            pltpu.VMEM((8,) + block, jnp.bfloat16),
            pltpu.VMEM((7,) + block, jnp.bfloat16),
            pltpu.VMEM((7,) + block, jnp.bfloat16),
            pltpu.VMEM((8,) + block, jnp.bfloat16),
            pltpu.SemaphoreType.DMA((4, 2 * z_count - 1)),
            pltpu.SemaphoreType.DMA((4, fs_count)),
            pltpu.SemaphoreType.DMA((4,)),
            pltpu.SemaphoreType.DMA((2, 7)),
            pltpu.SemaphoreType.DMA((2, 8)),
            pltpu.SemaphoreType.DMA((2,)),
            pltpu.SemaphoreType.DMA((2, 7)),
            pltpu.SemaphoreType.DMA((2, 7)),
            pltpu.VMEM((2, rows, hidden_half), jnp.float32),
            pltpu.VMEM((2, rows, hidden_half), jnp.bfloat16),
            pltpu.VMEM(block, jnp.bfloat16),
        ],
        compiler_params=pltpu.CompilerParams(
            collective_id=0, has_side_effects=True, vmem_limit_bytes=60 * 1024 * 1024
        ),
        name="layer",
    )(
        tokens,
        norm_in_gain.reshape(1, -1),
        norm_mid_gain.reshape(1, -1),
        wa,
        wg,
        wv,
        wd,
        taps,
        bias,
        jnp.asarray(cosine),
        jnp.asarray(sine),
        jnp.asarray(turn, jnp.bfloat16),
    )


def solution(mesh):
    fs_count, tp_count = mesh.shape["fs"], mesh.shape["tp"]

    def step(*args):
        local_heads = args[2].shape[1] // HEAD_DIM
        if local_heads == 2 and tp_count == 4 and fs_count == 8:
            return fused(fs_count, local_heads * tp_count, *args)
        return local(*args)

    return jax.shard_map(
        step,
        mesh=mesh,
        in_specs=(
            P("fs", "tp"),
            P(),
            P("fs", "tp"),
            P("fs", "tp"),
            P("fs", "tp"),
            P("fs", "tp"),
            P("tp", "fs"),
            P(),
            P("fs", "tp"),
            P("fs", "tp"),
            P(None, "tp"),
            P("tp"),
            P("tp", "fs"),
        ),
        out_specs=P("fs", "tp"),
        check_vma=False,
    )
```

```python
import jax
import jax.numpy as jnp
import numpy as np
from jax import lax
from jax.experimental import pallas as pl
from jax.experimental.pallas import tpu as pltpu
from jax.sharding import PartitionSpec as P

BLOCK = 32
HEAD_DIM = 96


epsilon = 1e-06
rotary_base = 10000.0


def taken_in(shard, axis, dim, absorb, state):
    everything = jax.tree.map(lambda a: lax.all_gather(a, axis, axis=dim, tiled=True), shard)
    return absorb(state, everything, jnp.int32(0))


def gathered_then(shard, axis, dim, block):
    whole = lax.all_gather(shard, axis, axis=dim, tiled=True)
    return block(whole, jnp.int32(0))


def rms_scale(row_block, gain_row):
    widened = row_block.astype(jnp.float32)
    scaled = widened * lax.rsqrt(jnp.mean(widened * widened, axis=-1, keepdims=True) + epsilon)
    return (scaled * gain_row).astype(jnp.bfloat16)


def rotate(values_in, positions):
    half_width = values_in.shape[-1] // 2
    inv_freq = jnp.power(rotary_base, -jnp.arange(half_width, dtype=jnp.float32) / half_width)
    angles = positions[:, None] * inv_freq[None, :]
    cosine = jnp.cos(angles)[:, None, :]
    sine = jnp.sin(angles)[:, None, :]
    widened = values_in.astype(jnp.float32)
    first_half = widened[..., :half_width]
    second_half = widened[..., half_width:]
    return jnp.concatenate(
        [first_half * cosine - second_half * sine, first_half * sine + second_half * cosine],
        axis=-1,
    )


def retain(query_h, key_h, value_h, log_gamma, block_size):
    length, head_count, head_width = query_h.shape
    blocks = length // block_size
    offsets = jnp.arange(block_size, dtype=jnp.float32)
    lag_grid = offsets[:, None] - offsets[None, :]
    intra_decay = jnp.where(
        lag_grid[None] >= 0,
        jnp.exp(log_gamma[:, None, None] * jnp.maximum(lag_grid, 0.0)[None]),
        0.0,
    )
    query_decay = jnp.exp(log_gamma[None, :] * (offsets + 1.0)[:, None])
    key_decay = jnp.exp(log_gamma[None, :] * (block_size - 1.0 - offsets)[:, None])
    block_decay = jnp.exp(log_gamma * block_size)
    query_b = query_h.astype(jnp.float32).reshape(blocks, block_size, head_count, head_width)
    key_b = key_h.astype(jnp.float32).reshape(blocks, block_size, head_count, head_width)
    value_b = value_h.astype(jnp.float32).reshape(blocks, block_size, head_count, head_width)
    scores = (
        jnp.einsum("nchd,nshd->nhcs", query_b, key_b, precision=lax.Precision.HIGHEST)
        * intra_decay[None]
    )
    within = jnp.einsum("nhcs,nshe->nche", scores, value_b, precision=lax.Precision.HIGHEST)

    def advance(memory, block_inputs):
        query_n, key_n, value_n = block_inputs
        across_n = jnp.einsum(
            "chd,hde->che",
            query_n * query_decay[:, :, None],
            memory,
            precision=lax.Precision.HIGHEST,
        )
        memory = memory * block_decay[:, None, None] + jnp.einsum(
            "chd,che->hde", key_n * key_decay[:, :, None], value_n, precision=lax.Precision.HIGHEST
        )
        return (memory, across_n)

    initial = jnp.zeros((head_count, head_width, head_width), jnp.float32)
    final_memory, across = lax.scan(advance, initial, (query_b, key_b, value_b))
    return (within + across).reshape(length, head_count, head_width)


def mix_heads(queries, key_m, value_m, gate_m, log_gamma, head_width, block_size):
    length = queries.shape[0]
    head_count = queries.shape[1] // head_width
    positions = jnp.arange(length, dtype=jnp.float32)
    query_r = rotate(queries.reshape(length, head_count, head_width), positions).astype(
        jnp.bfloat16
    )
    key_r = (
        rotate(key_m.reshape(length, head_count, head_width), positions) * head_width ** (-0.5)
    ).astype(jnp.bfloat16)
    retained = retain(
        query_r, key_r, value_m.reshape(length, head_count, head_width), log_gamma, block_size
    )
    normed = retained * lax.rsqrt(jnp.mean(retained * retained, axis=-1, keepdims=True) + epsilon)
    return (normed.reshape(length, -1) * jax.nn.silu(gate_m.astype(jnp.float32))).astype(
        jnp.bfloat16
    )


def convolve(gate_up, conv_taps, conv_bias):
    length = gate_up.shape[0]
    tap_count = conv_taps.shape[0]
    padded = jnp.pad(gate_up.astype(jnp.float32), ((tap_count - 1, 0), (0, 0)))
    summed = jnp.zeros(gate_up.shape, jnp.float32) + conv_bias[None, :]
    for tap_index in range(tap_count):
        summed = summed + padded[tap_index : tap_index + length] * conv_taps[tap_index][None, :]
    return summed


def single(normed):

    def add_single(running, weight_piece, row_start):
        columns = lax.dynamic_slice_in_dim(normed, row_start, weight_piece.shape[0], 1)
        return running + jnp.dot(columns, weight_piece, preferred_element_type=jnp.float32)

    return add_single


def features(shard):
    return lax.all_gather(shard, "tp", axis=1, tiled=True)


def head_sum(terms):
    return lax.psum_scatter(
        terms.astype(jnp.bfloat16), "tp", scatter_dimension=1, tiled=True
    ).astype(jnp.float32)


def local(
    tokens,
    norm_in_gain,
    query_w,
    key_w,
    value_w,
    gate_w,
    out_w,
    norm_mid_gain,
    up_gate_w,
    up_value_w,
    conv_taps,
    conv_bias,
    down_w,
):
    normed_in = rms_scale(features(tokens), norm_in_gain)
    length = normed_in.shape[0]

    def empty(weight):
        return jnp.zeros((length, weight.shape[1]), jnp.float32)

    add_in = single(normed_in)

    def mixer_row(weight):
        return taken_in(weight, "fs", 0, add_in, empty(weight))

    queries = mixer_row(query_w)
    key_m = mixer_row(key_w)
    value_m = mixer_row(value_w)
    gate_m = mixer_row(gate_w)
    head_count = query_w.shape[1] // HEAD_DIM
    first_head = lax.axis_index("tp") * head_count
    head_ids = (first_head + jnp.arange(head_count, dtype=jnp.int32)).astype(jnp.float32)
    log_gamma = jnp.log1p(-jnp.exp2(-5.0 - head_ids))
    gated_heads = mix_heads(
        queries.astype(jnp.bfloat16),
        key_m.astype(jnp.bfloat16),
        value_m.astype(jnp.bfloat16),
        gate_m.astype(jnp.bfloat16),
        log_gamma,
        HEAD_DIM,
        BLOCK,
    )

    def mixer_project(weight_piece, row_start):
        return jnp.dot(gated_heads, weight_piece, preferred_element_type=jnp.float32)

    mixer_terms = gathered_then(out_w, "fs", 1, mixer_project)
    middle = (tokens.astype(jnp.float32) + head_sum(mixer_terms)).astype(jnp.bfloat16)
    normed_mid = rms_scale(features(middle), norm_mid_gain)
    add_mid = single(normed_mid)

    def channel_row(weight):
        return taken_in(weight, "fs", 0, add_mid, empty(weight))

    gate_up = channel_row(up_gate_w)
    value_up = channel_row(up_value_w)
    convolved = convolve(gate_up.astype(jnp.bfloat16), conv_taps, conv_bias)
    hidden = (jax.nn.silu(convolved) * value_up.astype(jnp.bfloat16).astype(jnp.float32)).astype(
        jnp.bfloat16
    )

    def channel_project(weight_piece, row_start):
        return jnp.dot(hidden, weight_piece, preferred_element_type=jnp.float32)

    channel_terms = gathered_then(down_w, "fs", 1, channel_project)
    return (middle.astype(jnp.float32) + head_sum(channel_terms)).astype(jnp.bfloat16)


LANES = 128
MESH = pl.DeviceIdType.MESH


def dot(left, right):
    return jnp.dot(left, right, preferred_element_type=jnp.float32)


def dot_t(left, right):
    return lax.dot_general(left, right, (((1,), (1,)), ((), ())), preferred_element_type=jnp.float32)


def layer_kernel(
    fs_count,
    heads,
    *refs,
):
    count = 16
    sources, out_ref, local_refs, load_sem = refs[:count], refs[count], refs[count + 1 : 2 * count + 1], refs[2 * count + 1]
    layer_body(fs_count, heads, sources, local_refs, load_sem, out_ref, *refs[2 * count + 2 :])


def layer_body(
    fs_count,
    heads,
    sources,
    local_refs,
    load_sem,
    out_ref,
    wa_ref,
    wd_ref,
    ga,
    gg,
    gv,
    gd,
    tok_all,
    mid_all,
    part_mix,
    part_ch,
    land_mix,
    land_ch,
    normed,
    w_send,
    w_recv,
    w_own,
    ag_send,
    ag_recv,
    ag_own,
    rs_send,
    rs_recv,
    hidden_gate,
    hidden,
    middle,
    land_half,
):
    loads = [
        pltpu.make_async_copy(source, here, load_sem.at[i])
        for i, (source, here) in enumerate(zip(sources, local_refs))
    ]
    for load in loads:
        load.start()
    (
        tokens_ref,
        query_ref,
        key_ref,
        value_ref,
        gate_ref,
        o_ref,
        wg_ref,
        wv_ref,
        down_ref,
        gain_in_ref,
        gain_mid_ref,
        taps_ref,
        bias_ref,
        cos_ref,
        sin_ref,
        turn_ref,
    ) = local_refs
    fs = lax.axis_index("fs")
    tp = lax.axis_index("tp")
    z, x = fs // 2, fs % 2
    y, c = tp // 2, tp % 2
    zl = z % 2
    z_count = fs_count // 2
    rows, width = tokens_ref.shape
    depth = wa_ref.shape[1]
    tp_count = 4
    z_mate = (z + 1 - 2 * zl) * 2 + x
    x_mate = z * 2 + 1 - x
    y_mate = (1 - y) * 2 + c
    c_mate = y * 2 + 1 - c
    to_z, to_x, to_y, to_c = (z_mate, tp), (x_mate, tp), (fs, y_mate), (fs, c_mate)
    z_peers = [lax.rem(z + step, z_count) for step in range(1, z_count)]

    barrier = pltpu.get_barrier_semaphore()
    greeted = [(zp * 2 + x, tp) for zp in z_peers] + [to_x, to_y, to_c]
    for peer in greeted:
        pl.semaphore_signal(barrier, inc=1, device_id=peer, device_id_type=MESH)
    for load in loads[:6]:
        load.wait()
    hidden_half = wd_ref.shape[2]
    for b in range(2):
        head_rows = slice(b * HEAD_DIM, (b + 1) * HEAD_DIM)
        pieces = [w[...][:, head_rows] for w in (query_ref, key_ref, value_ref, gate_ref)]
        pieces.append(o_ref[head_rows].T)
        pieces.append(jnp.zeros((o_ref.shape[1], wa_ref.shape[2] - 5 * HEAD_DIM), jnp.bfloat16))
        wa_ref[b] = jnp.concatenate(pieces, axis=1)
    for load in loads[6:]:
        load.wait()
    pl.semaphore_wait(barrier, len(greeted))

    sends = []

    def remote(src, dst, send_sem, recv_sem, peer):
        copy = pltpu.make_async_remote_copy(
            src_ref=src,
            dst_ref=dst,
            send_sem=send_sem,
            recv_sem=recv_sem,
            device_id=peer,
            device_id_type=MESH,
        )
        copy.start()
        sends.append(copy)

    def arrived(ref, sem):
        pltpu.make_async_remote_copy(
            src_ref=ref,
            dst_ref=ref,
            send_sem=sem,
            recv_sem=sem,
            device_id=to_c,
            device_id_type=MESH,
        ).wait_recv()

    def slot(held, owner):
        return held.at[pl.ds(pl.multiple_of(owner * depth, depth), depth)]

    chunks = [(wa_ref, ga), (wg_ref, gg), (wv_ref, gv), (wd_ref, gd)]
    own_copies = []

    def weights_out(k):
        shard, held = chunks[k]

        def part(b):
            if k in (1, 2):
                start = pl.multiple_of(b * hidden_half, LANES)
                return shard.at[:, pl.ds(start, hidden_half)]
            return shard.at[b]

        for i, zp in enumerate(z_peers):
            remote(
                part(zp % 2),
                slot(held, fs),
                w_send.at[k, i],
                w_recv.at[k, fs],
                (zp * 2 + x, tp),
            )
        remote(
            part(zl), slot(held, fs), w_send.at[k, z_count - 1], w_recv.at[k, fs], to_x
        )
        own = pltpu.make_async_copy(part(zl), slot(held, fs), w_own.at[k])
        own.start()
        own_copies.append(own)

    def weights_on(k):
        held = chunks[k][1]
        for i in range(z_count - 1):
            owner = lax.rem(z + z_count - 1 - i, z_count) * 2 + x
            arrived(slot(held, owner), w_recv.at[k, owner])
            remote(
                slot(held, owner),
                slot(held, owner),
                w_send.at[k, z_count + i],
                w_recv.at[k, owner],
                to_x,
            )

    def weights_in(k):
        held = chunks[k][1]
        own_copies[k].wait()
        for step in range(z_count):
            owner = lax.rem(z + z_count - step, z_count) * 2 + 1 - x
            arrived(slot(held, owner), w_recv.at[k, owner])

    mine = zl * 4 + tp
    from_z = (1 - zl) * 4 + tp
    from_y = zl * 4 + y_mate
    from_zy = (1 - zl) * 4 + y_mate
    gathered = (mine, from_z, from_y, from_zy)

    def gather_start(phase, src, held):
        def pass_on(which, ref, block, peer):
            remote(
                ref, held.at[block], ag_send.at[phase, which], ag_recv.at[phase, block], peer
            )

        pass_on(0, src, mine, to_z)
        pass_on(1, src, mine, to_y)
        pass_on(2, src, mine, to_c)
        own = pltpu.make_async_copy(src, held.at[mine], ag_own.at[phase])
        own.start()
        return pass_on, own

    def gather_end(phase, held, state):
        pass_on, own = state
        arrived(held.at[from_z], ag_recv.at[phase, from_z])
        pass_on(3, held.at[from_z], from_z, to_y)
        pass_on(4, held.at[from_z], from_z, to_c)
        arrived(held.at[from_y], ag_recv.at[phase, from_y])
        pass_on(5, held.at[from_y], from_y, to_c)
        arrived(held.at[from_zy], ag_recv.at[phase, from_zy])
        pass_on(6, held.at[from_zy], from_zy, to_c)
        own.wait()
        for half in range(2):
            for side in range(2):
                block = half * 4 + side * 2 + 1 - c
                arrived(held.at[block], ag_recv.at[phase, block])

    def add_into(parts, block, land, where):
        parts[block] = (
            parts[block].astype(jnp.float32) + land[where].astype(jnp.float32)
        ).astype(jnp.bfloat16)

    def scatter(phase, parts, land, between, waiting):
        def give(which, block, peer):
            remote(
                parts.at[block],
                land.at[which],
                rs_send.at[phase, which],
                rs_recv.at[phase, which],
                peer,
            )

        def take(which):
            arrived(land.at[which], rs_recv.at[phase, which])

        for side in (1 - y, y):
            for half in (1 - zl, zl):
                give(half * 2 + side, half * 4 + side * 2 + 1 - c, to_c)
        for half in (1 - zl, zl):
            which = half * 2 + 1 - y
            take(which)
            block = half * 4 + (1 - y) * 2 + c
            add_into(parts, block, land, which)
            give(4 + half, block, to_y)
        between()
        for half in (1 - zl, zl):
            which = half * 2 + y
            take(which)
            add_into(parts, half * 4 + tp, land, which)
        take(4 + 1 - zl)
        add_into(parts, from_z, land, 4 + 1 - zl)
        give(6, from_z, to_z)
        waiting()
        take(4 + zl)
        total = parts[mine].astype(jnp.float32) + land[4 + zl].astype(jnp.float32)
        take(6)
        return total + land[6].astype(jnp.float32)

    def scatter_out(parts, land):
        top, low = pl.ds(0, rows // 2), pl.ds(rows // 2, rows // 2)

        def give(which, src, dst, peer):
            remote(src, dst, rs_send.at[1, which], rs_recv.at[1, which], peer)

        def give_half(which, block, part, peer):
            give(4 + which, parts.at[block, part], land_half.at[which], peer)

        def take(which, ref):
            arrived(ref, rs_recv.at[1, which])

        def take_half(which):
            take(4 + which, land_half.at[which])
            return land_half[which].astype(jnp.float32)

        for half, side in ((1 - zl, 1 - y), (zl, 1 - y), (1 - zl, y), (zl, y)):
            which = half * 2 + side
            give(which, parts.at[half * 4 + side * 2 + 1 - c], land.at[which], to_c)

        def settle(half, side):
            which = half * 2 + side
            take(which, land.at[which])
            add_into(parts, half * 4 + side * 2 + c, land, which)

        settle(1 - zl, 1 - y)
        give_half(0, from_zy, top, to_y)
        give_half(3, from_zy, low, to_z)
        settle(zl, 1 - y)
        give_half(1, from_y, top, to_y)
        settle(1 - zl, y)
        give_half(4, from_z, low, to_z)
        settle(zl, y)
        parts[from_z, top] = (parts[from_z, top].astype(jnp.float32) + take_half(0)).astype(
            jnp.bfloat16
        )
        give_half(2, from_z, top, to_z)
        parts[from_y, low] = (parts[from_y, low].astype(jnp.float32) + take_half(3)).astype(
            jnp.bfloat16
        )
        give_half(5, from_y, low, to_y)
        base = middle[...].astype(jnp.float32) + parts[mine].astype(jnp.float32)
        upper = base[: rows // 2] + take_half(1)
        lower = base[rows // 2 :] + take_half(4)
        out_ref[top] = (upper + take_half(2)).astype(jnp.bfloat16)
        out_ref[low] = (lower + take_half(5)).astype(jnp.bfloat16)

    def normalise(held, gain_ref):
        @pl.loop(0, 2)
        def _(half):
            squares = jnp.zeros((rows, 1), jnp.float32)
            for t in range(tp_count):
                wide = held[half * 4 + t].astype(jnp.float32)
                squares = squares + jnp.sum(wide * wide, axis=-1, keepdims=True)
            scale = lax.rsqrt(squares / (tp_count * width) + epsilon)
            for t in range(tp_count):
                wide = held[half * 4 + t].astype(jnp.float32)
                normed[half * 4 + t] = (
                    wide * scale * gain_ref[t * width : (t + 1) * width][None, :]
                ).astype(jnp.bfloat16)

    def project(half, held, columns):
        total = dot(normed[half * 4], held[0:width, 0:columns])
        for t in range(1, tp_count):
            total = total + dot(
                normed[half * 4 + t], held[t * width : (t + 1) * width, 0:columns]
            )
        return total.astype(jnp.bfloat16)

    state = gather_start(0, tokens_ref, tok_all)
    weights_out(0)
    weights_out(1)
    weights_out(2)
    for b in range(2):
        wd_ref[b] = down_ref[b * hidden_half : (b + 1) * hidden_half].T
    weights_out(3)
    gather_end(0, tok_all, state)
    normalise(tok_all, gain_in_ref)
    weights_on(0)
    weights_in(0)

    head = tp * 2 + zl
    log_gamma = jnp.float32(0.0)
    for j in range(heads):
        log_gamma = jnp.where(head == j, jnp.float32(np.log1p(-(2.0 ** (-5.0 - j)))), log_gamma)

    @pl.loop(0, 2)
    def _(half):
        wide = project(half, ga, ga.shape[1])
        turn = turn_ref[...]

        def rotated(piece):
            return piece.astype(jnp.float32) * cos_ref[...] + dot(piece, turn) * sin_ref[...]

        query_r = rotated(wide[:, 0 * HEAD_DIM : 1 * HEAD_DIM]).astype(jnp.bfloat16)
        key_r = (rotated(wide[:, 1 * HEAD_DIM : 2 * HEAD_DIM]) * HEAD_DIM ** (-0.5)).astype(jnp.bfloat16)
        value = wide[:, 2 * HEAD_DIM : 3 * HEAD_DIM]
        gate = wide[:, 3 * HEAD_DIM : 4 * HEAD_DIM].astype(jnp.float32)
        later = lax.broadcasted_iota(jnp.int32, (rows, rows), 0)
        earlier = lax.broadcasted_iota(jnp.int32, (rows, rows), 1)
        lag = later - earlier
        decay = jnp.where(
            lag >= 0, jnp.exp(log_gamma * jnp.maximum(lag, 0).astype(jnp.float32)), 0.0
        )
        scores = dot_t(query_r, key_r) * decay
        coarse = scores.astype(jnp.bfloat16)
        fine = (scores - coarse.astype(jnp.float32)).astype(jnp.bfloat16)
        retained = dot(coarse, value) + dot(fine, value)
        square = jnp.sum(retained * retained, axis=-1, keepdims=True) / HEAD_DIM
        gated = (
            retained * lax.rsqrt(square + epsilon) * (gate * (1.0 / (1.0 + jnp.exp(-gate))))
        ).astype(jnp.bfloat16)
        for t in range(tp_count):
            part_mix[half * 4 + t] = dot_t(
                gated, ga[t * width : (t + 1) * width, 4 * HEAD_DIM : 5 * HEAD_DIM]
            ).astype(jnp.bfloat16)

    mixed = scatter(0, part_mix, land_mix, lambda: (weights_on(1)), lambda: (weights_on(2)))
    middle[...] = (tokens_ref[...].astype(jnp.float32) + mixed).astype(jnp.bfloat16)
    state = gather_start(1, middle, mid_all)
    weights_on(3)
    gather_end(1, mid_all, state)
    normalise(mid_all, gain_mid_ref)
    weights_in(1)

    @pl.loop(0, 2)
    def _(half):
        up = project(half, gg, gg.shape[1]).astype(jnp.float32)
        at = lax.broadcasted_iota(jnp.int32, up.shape, 0)
        taps = taps_ref[:, pl.ds(pl.multiple_of(zl * hidden_half, LANES), hidden_half)]
        tap_count = taps.shape[0]
        summed = up * taps[tap_count - 1 : tap_count] + bias_ref[pl.ds(pl.multiple_of(zl * hidden_half, LANES), hidden_half)][None, :]
        for back in range(1, tap_count):
            moved = jnp.where(at >= back, pltpu.roll(up, back, 0), 0.0)
            summed = summed + moved * taps[tap_count - 1 - back : tap_count - back]
        hidden_gate[half] = summed * (1.0 / (1.0 + jnp.exp(-summed)))

    weights_in(2)

    @pl.loop(0, 2)
    def _(half):
        value_up = project(half, gv, gv.shape[1]).astype(jnp.float32)
        hidden[half] = (hidden_gate[half] * value_up).astype(jnp.bfloat16)

    weights_in(3)

    @pl.loop(0, 2)
    def _(half):
        for t in range(tp_count):
            part_ch[half * 4 + t] = dot_t(
                hidden[half], gd[t * width : (t + 1) * width]
            ).astype(jnp.bfloat16)

    scatter_out(part_ch, land_ch)
    for copy in sends:
        copy.wait_send()


def rotation_tables(length):
    half_width = HEAD_DIM // 2
    inv_freq = rotary_base ** (-np.arange(half_width) / half_width)
    angles = np.arange(length)[:, None] * inv_freq[None, :]
    angles = np.concatenate([angles, angles], axis=1)
    turn = np.zeros((HEAD_DIM, HEAD_DIM), np.float32)
    for i in range(half_width):
        turn[i + half_width, i] = -1.0
        turn[i, i + half_width] = 1.0
    return np.cos(angles).astype(np.float32), np.sin(angles).astype(np.float32), turn


def fused(
    fs_count,
    heads,
    tokens,
    norm_in_gain,
    query_w,
    key_w,
    value_w,
    gate_w,
    out_w,
    norm_mid_gain,
    up_gate_w,
    up_value_w,
    conv_taps,
    conv_bias,
    down_w,
):
    rows, width = tokens.shape
    hidden_half = up_gate_w.shape[1] // 2

    cosine, sine, turn = rotation_tables(rows)
    depth = query_w.shape[0]
    features_all = depth * fs_count
    first = -(-5 * HEAD_DIM // LANES) * LANES
    block = (rows, width)

    def held(columns):
        return pltpu.VMEM((features_all, columns), jnp.bfloat16)

    operands = (
        tokens,
        query_w,
        key_w,
        value_w,
        gate_w,
        out_w,
        up_gate_w,
        up_value_w,
        down_w,
        norm_in_gain,
        norm_mid_gain,
        conv_taps,
        conv_bias,
        jnp.asarray(cosine),
        jnp.asarray(sine),
        jnp.asarray(turn, jnp.bfloat16),
    )

    z_count = fs_count // 2
    return pl.pallas_call(
        lambda *refs: layer_kernel(fs_count, heads, *refs),
        out_shape=jax.ShapeDtypeStruct(block, jnp.bfloat16),
        in_specs=[pl.BlockSpec(memory_space=pl.ANY)] * len(operands),
        out_specs=pl.BlockSpec(memory_space=pltpu.VMEM),
        scratch_shapes=[
            *[pltpu.VMEM(array.shape, array.dtype) for array in operands],
            pltpu.SemaphoreType.DMA((len(operands),)),
            pltpu.VMEM((2, depth, first), jnp.bfloat16),
            pltpu.VMEM((2, depth, hidden_half), jnp.bfloat16),
            held(first),
            held(hidden_half),
            held(hidden_half),
            held(hidden_half),
            pltpu.VMEM((8,) + block, jnp.bfloat16),
            pltpu.VMEM((8,) + block, jnp.bfloat16),
            pltpu.VMEM((8,) + block, jnp.bfloat16),
            pltpu.VMEM((8,) + block, jnp.bfloat16),
            pltpu.VMEM((7,) + block, jnp.bfloat16),
            pltpu.VMEM((7,) + block, jnp.bfloat16),
            pltpu.VMEM((8,) + block, jnp.bfloat16),
            pltpu.SemaphoreType.DMA((4, 2 * z_count - 1)),
            pltpu.SemaphoreType.DMA((4, fs_count)),
            pltpu.SemaphoreType.DMA((4,)),
            pltpu.SemaphoreType.DMA((2, 7)),
            pltpu.SemaphoreType.DMA((2, 8)),
            pltpu.SemaphoreType.DMA((2,)),
            pltpu.SemaphoreType.DMA((2, 10)),
            pltpu.SemaphoreType.DMA((2, 10)),
            pltpu.VMEM((2, rows, hidden_half), jnp.float32),
            pltpu.VMEM((2, rows, hidden_half), jnp.bfloat16),
            pltpu.VMEM(block, jnp.bfloat16),
            pltpu.VMEM((6, rows // 2, width), jnp.bfloat16),
        ],
        compiler_params=pltpu.CompilerParams(
            collective_id=0, has_side_effects=True, vmem_limit_bytes=60 * 1024 * 1024
        ),
        name="layer",
    )(*operands)


def solution(mesh):
    fs_count, tp_count = mesh.shape["fs"], mesh.shape["tp"]

    def step(*args):
        local_heads = args[2].shape[1] // HEAD_DIM
        if local_heads == 2 and tp_count == 4 and fs_count == 8:
            return fused(fs_count, local_heads * tp_count, *args)
        return local(*args)

    return jax.shard_map(
        step,
        mesh=mesh,
        in_specs=(
            P("fs", "tp"),
            P(),
            P("fs", "tp"),
            P("fs", "tp"),
            P("fs", "tp"),
            P("fs", "tp"),
            P("tp", "fs"),
            P(),
            P("fs", "tp"),
            P("fs", "tp"),
            P(None, "tp"),
            P("tp"),
            P("tp", "fs"),
        ),
        out_specs=P("fs", "tp"),
        check_vma=False,
    )
```
